512 devices in a mesh: ep: 32 (over z, core), tp: 16 (over y, x).
Axes of the slice: x: 4, y: 4, z: 16, core: 2. Of those that a mesh axis runs over, the one named last changes fastest.
Arguments:
- queries: bfloat16 [8192, 2048], P('ep', 'tp'), may hold values from -6 to 6
- key_rows: bfloat16 [8192, 1024], P('ep', 'tp'), may hold values from -6 to 6
- values: bfloat16 [8192, 1024], P('ep', 'tp'), may hold values from -140 to 140
- query_gain: float32 [64], replicated, may hold values from 0.55 to 7.5
- key_gain: float32 [64], replicated, may hold values from 0.55 to 7.5
- mix_gain: float32 [2048], replicated, may hold values from 0.1 to 1.9
- out_weight: bfloat16 [2048, 4096], P(None, 'tp'), may hold values from -0.125 to 0.125
- expert_input: bfloat16 [8192, 4096], P('ep', 'tp'), may hold values from -140 to 140
- expert_gain: float32 [4096], replicated, may hold values from 0.1 to 1.9
- route_ids: int32 [8192, 2], P('ep'), may hold values from 0 to 31, as said below
- route_weights: float32 [8192, 2], P('ep'), may hold values from 0.3 to 1.7
- expert_gate: bfloat16 [32, 4096, 2048], P('ep', None, 'tp'), may hold values from -0.09375 to 0.09375
- expert_up: bfloat16 [32, 4096, 2048], P('ep', None, 'tp'), may hold values from -0.09375 to 0.09375
- expert_down: bfloat16 [32, 2048, 4096], P('ep', None, 'tp'), may hold values from -0.125 to 0.125
Outputs:
- attended: bfloat16 [8192, 4096], P('ep', 'tp')
- expert_mix: bfloat16 [8192, 4096], P('ep', 'tp')
The draws below stay inside these ranges and needn't reach their ends.
Inputs may be any that keep to these rules, and one draw needn't show every extreme that they name: `route_ids`: the 2 experts of a row differ. In every aligned block of 256 rows no expert is named more than 22 times, and one expert, the same for all blocks, is named exactly 22 times in every block.
All inputs are finite; a program needn't handle non-finite values.
Results may differ from the reference program's by a relative error of at most 0.01.
The reference program's roundings to bfloat16 on the way count: a program that leaves them out, or rounds other values in their place, can miss the bound.
Values may be sent and summed in bfloat16 or wider, within the bound.
A program may use at most 64 MiB of HBM per device.

```python
import math
import jax
import jax.numpy as jnp
from jax import lax

D = 4096
Q_HEADS = 32
KV_HEADS = 16
HEAD = 64
FF = 2048
TOP_K = 2
GRID_W = 64
TOK_DEV = 256
TOKENS = 8192
EXPERTS = 32
CAP = 22
N_EP = 32


def draw_key_rows(key, part):
    field_data = jnp.clip(jax.random.normal(jax.random.fold_in(key, 7), (TOKENS, KV_HEADS * HEAD), jnp.float32), -6.0, 6.0)
    return field_data.astype(jnp.bfloat16)


def draw_queries(key, part):
    field_data = jnp.clip(jax.random.normal(jax.random.fold_in(key, 9), (TOKENS, Q_HEADS * HEAD), jnp.float32), -6.0, 6.0)
    return field_data.astype(jnp.bfloat16)


def rising_field(seed_key, row_count, column_count, group_width):
    pieces = jax.random.split(seed_key, 2)
    group_count = column_count // group_width
    position = (jnp.arange(column_count) // group_width).astype(jnp.float32) / max(group_count - 1, 1)
    jitter = jax.random.uniform(pieces[1], (column_count,), jnp.float32)
    log_scale = math.log(10.0) * 0.5 * (position + jitter)
    field_data = jnp.clip(jax.random.normal(pieces[0], (row_count, column_count), jnp.float32), -4.0, 4.0)
    return field_data * jnp.exp(log_scale)


def draw_values(key, part):
    return rising_field(jax.random.fold_in(key, 3), TOKENS, KV_HEADS * HEAD, HEAD).astype(jnp.bfloat16)


def draw_expert_input(key, part):
    return rising_field(jax.random.fold_in(key, 5), TOKENS, D, 1).astype(jnp.bfloat16)


def draw_query_gain(key, part):
    seed_key = jax.random.fold_in(key, 21)
    return jax.random.uniform(seed_key, (HEAD,), jnp.float32, 0.55, 1.45)


def draw_key_gain(key, part):
    seed_key = jax.random.fold_in(key, 23)
    return jax.random.uniform(seed_key, (HEAD,), jnp.float32, 0.55, 1.45)


def block_routes(seed_key, favored):
    ticket_total = TOK_DEV * TOP_K
    pieces = jax.random.split(seed_key, 3)
    ticket_order = jax.random.permutation(pieces[0], (EXPERTS - 1) * CAP)
    live_slots = (ticket_order < ticket_total - CAP).astype(jnp.int32).reshape(EXPERTS - 1, CAP)
    rest_counts = jnp.sum(live_slots, axis=1).astype(jnp.int32)
    everyone = jnp.arange(EXPERTS, dtype=jnp.int32)
    rest_index = jnp.clip(everyone - (everyone > favored).astype(jnp.int32), 0, max(EXPERTS - 2, 0))
    counts = jnp.where(everyone == favored, CAP, rest_counts[rest_index]).astype(jnp.int32)
    run_order = jax.random.permutation(pieces[1], EXPERTS).astype(jnp.int32)
    run_ends = jnp.cumsum(counts[run_order]).astype(jnp.int32)
    run_index = jnp.searchsorted(run_ends, jnp.arange(ticket_total, dtype=jnp.int32), side='right')
    tickets = run_order[run_index]
    by_row = tickets.reshape(TOP_K, TOK_DEV).T
    row_order = jax.random.permutation(pieces[2], TOK_DEV)
    return jnp.zeros((TOK_DEV, TOP_K), jnp.int32).at[row_order].set(by_row)


def draw_route_ids(key, part):
    base_key = jax.random.fold_in(key, 13)
    favored = jax.random.randint(jax.random.fold_in(base_key, 1), (), 0, EXPERTS).astype(jnp.int32)
    block_keys = jax.random.split(jax.random.fold_in(base_key, 2), N_EP)
    routes = jax.vmap(block_routes, in_axes=(0, None))(block_keys, favored)
    return routes.reshape(TOKENS, TOP_K).astype(jnp.int32)


def steps_of(key, extent, shards, least, high):
    def one(dim, parts):
        draws = jax.random.uniform(jax.random.fold_in(jax.random.fold_in(key, 6), dim), (parts,), jnp.float32, least / len(shards), high / len(shards))
        return jnp.repeat(jnp.exp(draws), extent[dim] // parts).reshape((-1,) + (1,) * (len(extent) - dim - 1))

    gain = one(*shards[0])
    for cut in shards[1:]:
        gain = gain * one(*cut)
    return gain


def scatter_about(own_key, dims, spread, limit, cuts=(), held_as=jnp.bfloat16):
    loudness = steps_of(own_key, dims, cuts, -0.22, 0.18) if cuts else 1.0
    result = jax.random.normal(own_key, dims, jnp.float32) * spread * loudness
    return jnp.minimum(jnp.maximum(result, -limit), limit).astype(held_as)


def setup_inputs(seed: int = 0) -> dict:
    key_of = jax.random.split(jax.random.key(seed), 15)
    queries = draw_queries(jax.random.fold_in(key_of[14], 71), 0)
    key_rows = draw_key_rows(jax.random.fold_in(key_of[14], 71), 0)
    values = draw_values(jax.random.fold_in(key_of[14], 71), 0)
    query_gain = draw_query_gain(jax.random.fold_in(key_of[14], 71), 0)
    key_gain = draw_key_gain(jax.random.fold_in(key_of[14], 71), 0)
    mix_gain = jnp.clip(1.0 + 0.18 * jax.random.normal(key_of[5], (Q_HEADS * HEAD,), jnp.float32), 0.1, 1.9)
    out_weight = scatter_about(key_of[6], (Q_HEADS * HEAD, D), (Q_HEADS * HEAD) ** -0.5, 0.125, ((1, 16),))
    expert_input = draw_expert_input(jax.random.fold_in(key_of[14], 71), 0)
    expert_gain = jnp.clip(1.0 + 0.18 * jax.random.normal(key_of[8], (D,), jnp.float32), 0.1, 1.9)
    route_ids = draw_route_ids(jax.random.fold_in(key_of[14], 71), 0)
    route_weights = jnp.clip(0.3 + 1.40000004 * jax.random.uniform(key_of[10], (TOKENS, TOP_K), jnp.float32) ** steps_of(key_of[10], (TOKENS, TOP_K), ((0, 32),), -0.2, 0.2), 0.3, 1.7)
    expert_gate = scatter_about(key_of[11], (EXPERTS, D, FF), D ** -0.5, 0.09375, ((0, 32), (2, 16)))
    expert_up = scatter_about(key_of[12], (EXPERTS, D, FF), D ** -0.5, 0.09375, ((0, 32), (2, 16)))
    expert_down = scatter_about(key_of[13], (EXPERTS, FF, D), FF ** -0.5, 0.125, ((0, 32), (2, 16)))
    return dict(queries=queries, key_rows=key_rows, values=values, query_gain=query_gain, key_gain=key_gain, mix_gain=mix_gain, out_weight=out_weight, expert_input=expert_input, expert_gain=expert_gain, route_ids=route_ids, route_weights=route_weights, expert_gate=expert_gate, expert_up=expert_up, expert_down=expert_down)


EPS = 1e-06
THETA = 10000.0

def turn_tables(length):
    half_width = HEAD // 2
    inverse = THETA ** (-jnp.arange(0, half_width, 2, dtype=jnp.float32) / half_width)
    positions = jnp.arange(length, dtype=jnp.int32)
    grid_rows = (positions // GRID_W).astype(jnp.float32)
    grid_cols = (positions % GRID_W).astype(jnp.float32)
    angles = jnp.concatenate([grid_rows[:, None] * inverse, grid_cols[:, None] * inverse], axis=-1)
    return (jnp.cos(angles), jnp.sin(angles))

def norm_turn(source, scale_gain, cosine_table, sine_table):
    length = source.shape[0]
    head_rows = source.astype(jnp.float32).reshape(length, -1, HEAD)
    head_rows = head_rows * lax.rsqrt(lax.optimization_barrier(jnp.mean(head_rows * head_rows, axis=-1, keepdims=True)) + EPS) * scale_gain
    pair_view = head_rows.reshape(length, head_rows.shape[1], HEAD // 2, 2)
    even_part = pair_view[..., 0]
    odd_part = pair_view[..., 1]
    cosine_part = cosine_table[:, None, :]
    sine_part = sine_table[:, None, :]
    turned = jnp.stack([even_part * cosine_part - odd_part * sine_part, even_part * sine_part + odd_part * cosine_part], axis=-1)
    return turned.reshape(length, -1).astype(jnp.bfloat16)

def attend_head(operands):
    query_group, key_head, value_head = operands
    length = query_group.shape[0]
    block_rows = math.gcd(length, 512)
    query_blocks = query_group.reshape(length // block_rows, block_rows, query_group.shape[1], HEAD)
    keys_float = key_head.astype(jnp.float32)
    values_float = value_head.astype(jnp.float32)

    def one_block(query_block):
        scores = jnp.einsum('rgd,nd->grn', query_block.astype(jnp.float32), keys_float) / math.sqrt(HEAD)
        row_max = lax.optimization_barrier(jnp.max(scores, axis=-1, keepdims=True))
        raw_weights = jnp.exp(scores - row_max)
        row_total = lax.optimization_barrier(jnp.sum(raw_weights, axis=-1))
        rounded = lax.optimization_barrier(raw_weights.astype(jnp.bfloat16)).astype(jnp.float32)
        summed = jnp.einsum('grn,nd->rgd', rounded, values_float)
        return (summed / jnp.transpose(row_total)[:, :, None]).astype(jnp.bfloat16)
    return lax.map(one_block, query_blocks).reshape(length, -1)

def reference(queries, key_rows, values, query_gain, key_gain, mix_gain, out_weight, expert_input, expert_gain, route_ids, route_weights, expert_gate, expert_up, expert_down):
    length = queries.shape[0]
    cosine_table, sine_table = turn_tables(length)
    query_turned = norm_turn(queries, query_gain, cosine_table, sine_table)
    key_turned = norm_turn(key_rows, key_gain, cosine_table, sine_table)
    group_size = Q_HEADS // KV_HEADS
    query_heads = query_turned.reshape(length, KV_HEADS, group_size, HEAD).transpose(1, 0, 2, 3)
    key_heads = key_turned.reshape(length, KV_HEADS, HEAD).transpose(1, 0, 2)
    value_heads = values.reshape(length, KV_HEADS, HEAD).transpose(1, 0, 2)
    heads_out = lax.map(attend_head, (query_heads, key_heads, value_heads))
    heads_out = heads_out.transpose(1, 0, 2).reshape(length, Q_HEADS * HEAD)
    heads_float = heads_out.astype(jnp.float32)
    mix_scale = lax.rsqrt(lax.optimization_barrier(jnp.mean(heads_float * heads_float, axis=-1)) + EPS)
    mix_in = (heads_float * mix_gain).astype(jnp.bfloat16)
    attended = (jnp.dot(mix_in, out_weight, preferred_element_type=jnp.float32) * mix_scale[:, None]).astype(jnp.bfloat16)
    blocks = N_EP
    copies = TOK_DEV * TOP_K
    ids_block = route_ids.reshape(blocks, copies).astype(jnp.int32)
    hit_marks = (ids_block[:, :, None] == jnp.arange(EXPERTS, dtype=jnp.int32)[None, None, :]).astype(jnp.int32)
    earlier = (jnp.cumsum(hit_marks, axis=1) - hit_marks).astype(jnp.int32)
    places = lax.optimization_barrier(jnp.sum(earlier * hit_marks, axis=2)).astype(jnp.int32)
    block_index = jnp.broadcast_to(jnp.arange(blocks, dtype=jnp.int32)[:, None], (blocks, copies))
    token_index = block_index * TOK_DEV + (jnp.arange(copies, dtype=jnp.int32) // TOP_K)[None, :]
    slot_table = jnp.full((EXPERTS, blocks, CAP), length, jnp.int32)
    slot_table = slot_table.at[ids_block, block_index, places].set(token_index.astype(jnp.int32))
    input_float = expert_input.astype(jnp.float32)
    expert_stat = lax.rsqrt(lax.optimization_barrier(jnp.mean(input_float * input_float, axis=-1)) + EPS)
    expert_scaled = (input_float * expert_gain).astype(jnp.bfloat16)
    scaled_pad = jnp.concatenate([expert_scaled, jnp.zeros((1, D), jnp.bfloat16)], axis=0)
    stat_pad = jnp.concatenate([expert_stat, jnp.zeros((1,), jnp.float32)], axis=0)

    def run_expert(operands):
        slot_tokens, gate_weight, up_weight, down_weight = operands
        flat_tokens = slot_tokens.reshape(-1)
        slot_input = scaled_pad[flat_tokens]
        row_stat = stat_pad[flat_tokens][:, None]
        gate_value = jnp.dot(slot_input, gate_weight, preferred_element_type=jnp.float32) * row_stat
        up_value = jnp.dot(slot_input, up_weight, preferred_element_type=jnp.float32) * row_stat
        hidden = (jax.nn.silu(gate_value) * up_value).astype(jnp.bfloat16)
        return jnp.dot(hidden, down_weight, preferred_element_type=jnp.float32).astype(jnp.bfloat16)
    outputs = lax.map(run_expert, (slot_table, expert_gate, expert_up, expert_down))
    picked = outputs[ids_block, block_index * CAP + places].astype(jnp.float32)
    weighted = picked * route_weights.reshape(blocks, copies)[:, :, None]
    expert_mix = lax.optimization_barrier(jnp.sum(weighted.reshape(length, TOP_K, D), axis=1)).astype(jnp.bfloat16)
    return (attended, expert_mix)
```

```python
import functools

import jax
import jax.numpy as jnp
import numpy as np
from jax import lax
from jax.experimental import pallas as pl
from jax.experimental.pallas import tpu as pltpu
from jax.sharding import Mesh
from jax.sharding import PartitionSpec as P

MESH = pl.DeviceIdType.MESH
EP = ("z", "c")
TP = ("y", "x")
HEAD = 64
GRID_W = 64
EPS = 1e-06
THETA = 10000.0
NZ = 16
NX = 4
TOK = 256
CAP = 22
PAD = 24
EXPERTS = 32
D = 4096
QDIM = 2048

OFFSETS = ((0, 1), (-1, 2), (3, -4), (5, -5), (6, -6), (7, -7), (8, 4), (-2, -3))
CHUNKS = len(OFFSETS)
BLOCKS = [(dz, dc) for part in OFFSETS for dz in part for dc in (0, 1)]
SPANS = [(2 * sum(map(len, OFFSETS[:n])), 2 * len(OFFSETS[n])) for n in range(CHUNKS)]
MOST = PAD * max(count for begin, count in SPANS)

ORDER = (
    "S1", "S0", "S7", "S5", "S6", "A1", "A0", "A7", "X11", "Q", "K0", "X01", "X12", "X02", "X71", "X72", "S2", "X13",
    "X04", "A5", "X03", "S3", "X73", "X74", "X14", "K1", "S4", "A6", "T0", "X51", "A2", "X05", "X75", "T1", "X15",
    "X52", "K2", "X61", "X53", "A3", "X21", "X62", "L0", "L1", "E7", "X22", "K3", "X63", "T2", "X54", "A4", "X55",
    "X31", "X23", "K4", "X65", "X64", "T3", "X41", "X42", "T4", "E5", "K5", "X24", "X33", "E6", "X43", "X44", "X25",
    "T5", "H51", "X34", "K6", "E1", "X45", "H61", "X35", "X32", "T6", "H53", "H72", "H54", "H71", "E2", "H52", "E4",
    "K7", "H55", "H64", "H63", "H11", "E3", "H73", "E0", "H41", "L2", "J5", "H42", "K8", "H62", "H65", "H21", "H74",
    "T7", "H75", "H31", "T8", "H43", "H13", "H44", "M0", "H12", "J6", "J7", "H34", "H33", "H23", "H45", "H22", "H15",
    "H01", "H32", "M2", "H02", "H35", "M1", "H24", "J4", "H04", "H14", "H25", "H03", "J3", "M4", "M3", "H05", "J2",
    "J1", "M5", "J0", "L3", "M6", "R",
)


def angle_tables():
    half = HEAD // 2
    inverse = (np.float32(THETA) ** (-np.arange(0, half, 2, dtype=np.float32) / np.float32(half))).astype(np.float32)
    angles = (np.arange(128, dtype=np.float32)[:, None] * inverse).astype(np.float32).astype(np.float64)
    pair = np.repeat(np.stack([np.cos(angles), np.sin(angles)]), 2, axis=2).astype(np.float32)
    pair[1, :, 0::2] *= -1
    none = np.zeros_like(pair)
    by_row = np.concatenate([pair, none, pair, none], axis=2)
    by_col = np.concatenate([none, pair, none, pair], axis=2)[:, :GRID_W]
    return by_row, by_col


def wrap(a, n):
    return lax.rem(a + n, n)


def norm_turn(x, gain, cosine, sine):
    low = lax.broadcasted_iota(jnp.int32, x.shape, 1) < HEAD
    squares = x * x
    first = jnp.sum(jnp.where(low, squares, 0.0), axis=1, keepdims=True)
    second = jnp.sum(jnp.where(low, 0.0, squares), axis=1, keepdims=True)
    x = x * lax.rsqrt(jnp.where(low, first, second) / HEAD + EPS) * gain
    even = lax.rem(lax.broadcasted_iota(jnp.int32, x.shape, 1), 2) == 0
    other = jnp.where(even, pltpu.roll(x, 127, 1), pltpu.roll(x, 1, 1))
    return x * cosine + other * sine


def dot(a, b, dims=((1,), (0,))):
    return lax.dot_general(a, b, (dims, ((), ())), preferred_element_type=jnp.float32)


def kernel(
    *refs,
):
    sources, (wo_hbm, wg_hbm, wu_hbm, wd_hbm) = refs[:12], refs[12:16]
    (att_ref, mix_ref), held = refs[16:18], refs[18:30]
    (
        gains, cs, q1, q2, kv, run_max, run_sum, run_acc, pick, out, xs, hs, ho, back, ret, acc, sq, wgu, wd, wo,
        sent, disp_r, ret_r, ag_r, kz_r, kd_r, w_s, own_s, in_s,
    ) = refs[30:]
    ids_ref, x_ref, q_ref, kt_ref, vt_ref, qg_ref, kg_ref, byrow_ref, bycol_ref, mg_ref, eg_ref, rw_ref = held
    z, c = lax.axis_index("z"), lax.axis_index("c")
    y, x = lax.axis_index("y"), lax.axis_index("x")
    coord = {"y": y, "x": x}

    barrier = pltpu.get_barrier_semaphore()

    def partner(dz, dc):
        return {"z": lax.rem(z + (dz + NZ), NZ), "c": lax.rem(c + dc, 2)}

    def side(axis, step):
        return {axis: lax.rem(coord[axis] + (step + NX), NX)}

    for dz, dc in BLOCKS[1:]:
        pl.semaphore_signal(barrier, inc=1, device_id=partner(dz, dc), device_id_type=MESH)
    for axis in ("x", "y"):
        for step in (1, -1):
            pl.semaphore_signal(barrier, inc=1, device_id=side(axis, step), device_id_type=MESH)

    inputs = [pltpu.make_async_copy(src, dst, in_s.at[k]) for k, (src, dst) in enumerate(zip(sources, held))]
    for load in inputs:
        load.start()
    loads = [
        pltpu.make_async_copy(wg_hbm.at[0], wgu.at[:, 0:128], w_s.at[0]),
        pltpu.make_async_copy(wu_hbm.at[0], wgu.at[:, 128:256], w_s.at[1]),
        pltpu.make_async_copy(wd_hbm.at[0], wd, w_s.at[2]),
        pltpu.make_async_copy(wo_hbm, wo, w_s.at[3]),
    ]

    for load in inputs[:2]:
        load.wait()
    for load in loads:
        load.start()

    experts = lax.broadcasted_iota(jnp.int32, (EXPERTS, TOK), 0)
    hits = [jnp.where(experts == ids_ref[k : k + 1, :], 1.0, 0.0) for k in range(2)]
    earlier = lax.broadcasted_iota(jnp.int32, (TOK, TOK), 0) < lax.broadcasted_iota(jnp.int32, (TOK, TOK), 1)
    before = dot((hits[0] + hits[1]).astype(jnp.bfloat16), jnp.where(earlier, 1.0, 0.0).astype(jnp.bfloat16))
    keys = [
        ids_ref[k : k + 1, :].astype(jnp.float32) * 32.0 + jnp.sum(hits[k] * before, axis=0, keepdims=True)
        for k in range(2)
    ]
    places = lax.broadcasted_iota(jnp.int32, (PAD, TOK), 0)
    for n in range(CHUNKS):
        wanted = []
        begin, count = SPANS[n]
        for dz, dc in BLOCKS[begin : begin + count]:
            to = partner(dz, dc)
            wanted.append((places + (to["z"] * 2 + to["c"]) * 32).astype(jnp.float32))
        wanted = jnp.concatenate(wanted, axis=0)
        rows = pl.ds(begin * PAD, count * PAD)
        marks = [jnp.where(wanted == keys[k], 1.0, 0.0) for k in range(2)]
        for k in range(2):
            pick[k, rows, :] = marks[k].astype(jnp.bfloat16)
        chosen = dot((marks[0] + marks[1]).astype(jnp.bfloat16), x_ref[...])
        for h in range(2):
            out[h, begin : begin + count] = (
                chosen[:, h * 128 : (h + 1) * 128].reshape(count, PAD, 128).astype(jnp.bfloat16)
            )

    pl.semaphore_wait(barrier, len(BLOCKS) - 1 + 4)

    def arrived(ref, sem):
        remote(ref, ref, sem, sem, partner(0, 1)).wait_recv()

    def left(ref, sem):
        remote(ref, ref, sem, sem, partner(0, 1)).wait_send()

    def remote(src, dst, send, recv, device):
        return pltpu.make_async_remote_copy(
            src_ref=src, dst_ref=dst, send_sem=send, recv_sem=recv, device_id=device, device_id_type=MESH
        )

    chunk_of = [n for n, (begin, count) in enumerate(SPANS) for k in range(count)]

    def dispatch(i):
        return remote(out.at[:, i], xs.at[:, 0, 0, i], sent.at[0], disp_r.at[chunk_of[i]], partner(*BLOCKS[i]))

    def giveback(i):
        dz, dc = BLOCKS[i]
        return remote(back.at[i], ret.at[i], sent.at[1], ret_r.at[0], partner(-dz, dc))

    own_out = pltpu.make_async_copy(out.at[:, 0], xs.at[:, 0, 0, 0], own_s.at[0])
    own_back = pltpu.make_async_copy(back.at[0], ret.at[0], own_s.at[1])

    def queries_and_keys():
        for load in inputs[2:]:
            load.wait()
        first_row = (z * 2 + c) * (TOK // GRID_W)
        for g in range(TOK // GRID_W):
            for t in range(2):
                cs[t, g * GRID_W : (g + 1) * GRID_W, :] = byrow_ref[t, pl.ds(first_row + g, 1), :] + bycol_ref[t]
        for t, ref in enumerate((qg_ref, kg_ref)):
            gains[t : t + 1, 0:HEAD] = ref[...]
            gains[t : t + 1, HEAD:128] = ref[...]
        low = lax.broadcasted_iota(jnp.int32, (128, 128), 1) < HEAD
        keys_raw = kt_ref[...].astype(jnp.float32)
        keys_raw = jnp.concatenate([keys_raw[:, 0:128], keys_raw[:, 128:256]], axis=0).T
        kv[0, 0, 0:128, :] = norm_turn(
            keys_raw, gains[1:2, :], jnp.where(low, cs[0, 0:128], cs[0, 128:256]), jnp.where(low, cs[1, 0:128], cs[1, 128:256])
        ).astype(jnp.bfloat16)
        kv[0, 0, 128:192, :] = vt_ref[:, 0:128]
        kv[0, 0, 192:256, :] = vt_ref[:, 128:256]
        turned = norm_turn(q_ref[...].astype(jnp.float32), gains[0:1, :], cs[0], cs[1])
        turned = turned.astype(jnp.bfloat16).astype(jnp.float32) * 0.125
        low = lax.broadcasted_iota(jnp.int32, (TOK, 128), 1) < HEAD
        crossed = pltpu.roll(turned, HEAD, 1)
        q1[0:TOK, :] = jnp.where(low, turned, 0.0).astype(jnp.bfloat16)
        q1[TOK:, :] = jnp.where(low, crossed, 0.0).astype(jnp.bfloat16)
        q2[0:TOK, :] = jnp.where(low, 0.0, crossed).astype(jnp.bfloat16)
        q2[TOK:, :] = jnp.where(low, 0.0, turned).astype(jnp.bfloat16)
        run_max[...] = jnp.full_like(run_max, -jnp.inf)
        run_sum[...] = jnp.zeros_like(run_sum)
        run_acc[...] = jnp.zeros_like(run_acc)

    def stage_s(n):
        for i in range(SPANS[n][0], sum(SPANS[n])):
            if i == 0:
                own_out.start()
            else:
                dispatch(i).start()

    kinds = (0, 0, 1, 1, 2, 2, 3, 3, 5, 5, 4, 4, 5, 5, 5, 5)

    def gather(buf, begin, count, half, index, send):
        inner, outer = ("x", "y") if half == 0 else ("y", "x")
        lo, hi, whole = pl.ds(begin, count // 2), pl.ds(begin + count // 2, count - count // 2), pl.ds(begin, count)

        def at(o, i, part=whole):
            return buf.at[half, o, i, part]

        def copy(k, src, dst, axis, step):
            return remote(src, dst, sent.at[send], ag_r.at[index, kinds[k]], side(axis, step))

        both = pl.ds(1, 2)
        return [
            copy(0, at(0, 0), at(0, 2), inner, 1),
            copy(1, at(0, 0), at(0, 1), inner, -1),
            copy(2, at(0, 0), at(2, 0), outer, 1),
            copy(3, at(0, 0), at(1, 0), outer, -1),
            copy(4, at(0, 2, lo), at(0, 3, lo), inner, 1),
            copy(5, at(0, 1, hi), at(0, 3, hi), inner, -1),
            copy(6, at(0, both), at(2, both), outer, 1),
            copy(7, at(0, both), at(1, both), outer, -1),
            copy(8, at(2, 0, lo), at(3, 0, lo), outer, 1),
            copy(9, at(1, 0, hi), at(3, 0, hi), outer, -1),
            copy(10, at(0, 3), at(2, 3), outer, 1),
            copy(11, at(0, 3), at(1, 3), outer, -1),
            copy(12, at(2, 1), at(3, 1), outer, 1),
            copy(13, at(1, 2), at(3, 2), outer, -1),
            copy(14, at(2, 3, lo), at(3, 3, lo), outer, 1),
            copy(15, at(1, 3, hi), at(3, 3, hi), outer, -1),
        ]

    def both_halves(buf, begin, count, index, send):
        part, middle = pl.ds(begin, count), pl.ds(1, 2)
        landed = (
            buf.at[:, 0, middle, part], buf.at[:, middle, 0, part], buf.at[:, 0, 3, part],
            buf.at[:, middle, middle, part], buf.at[:, middle, 3, part], buf.at[:, 3, :, part],
        )
        return [gather(buf, begin, count, h, index, send) for h in range(2)], landed, index

    gx = [both_halves(xs, *SPANS[n], n, 2) for n in range(CHUNKS)]
    gh = [both_halves(hs, SPANS[n][0] // 2, SPANS[n][1] // 2, CHUNKS + n, 3) for n in range(CHUNKS)]
    gm = both_halves(ho, 0, 128, CHUNKS * 2, 4)

    steps = ((0, 1, 2, 3), (4, 5, 6, 7), (8, 9), (10, 11), (12, 13), (14, 15), ())

    def go(pair, step):
        gathers, landed, index = pair
        if step:
            arrived(landed[step - 1], ag_r.at[index, step - 1])
        for g in gathers:
            for k in steps[step]:
                g[k].start()

    def slots(t):
        ry, rx = (r + r // 2 - 2 * (r // 3) for r in (wrap(t // NX - y, NX), wrap(lax.rem(t, NX) - x, NX)))
        return (ry, rx), (rx, ry)

    def stage_a(n):
        begin, count = SPANS[n]
        if n == 0:
            own_out.wait()
            begin, count = 1, count - 1
        arrived(xs.at[:, 0, 0, pl.ds(begin, count)], disp_r.at[n])
        go(gx[n], 0)

    def feed_forward(n):
        begin, count = SPANS[n]
        rows, part_rows = pl.ds(0, count * PAD), count * PAD // 2
        acc[rows, :] = jnp.zeros((count * PAD, 256), jnp.float32)
        sq[rows, :] = jnp.zeros((count * PAD, 128), jnp.float32)

        def body(g, carry):
            parts, squares = [], None
            for k in range(4):
                t = g * 4 + k
                for h, (o, i) in enumerate(slots(t)):
                    part = xs[h, o, i, begin : begin + count].astype(jnp.float32).reshape(count * PAD, 128)
                    squares = part * part if squares is None else squares + part * part
                    parts.append((part * eg_ref[pl.ds(2 * t + h, 1), :]).astype(jnp.bfloat16))
            sq[rows, :] += squares
            weight = wgu[pl.ds(pl.multiple_of(g * 1024, 1024), 1024), :]
            acc[rows, :] += dot(jnp.concatenate(parts, axis=1), weight)
            return carry

        lax.fori_loop(0, 4, body, 0)
        stat = lax.rsqrt(jnp.sum(sq[rows, :], axis=1, keepdims=True) / D + EPS)
        gate = acc[rows, 0:128] * stat
        up = acc[rows, 128:256] * stat
        hidden = gate / (1.0 + jnp.exp(-gate)) * up
        for h in range(2):
            own = hidden[h * part_rows : (h + 1) * part_rows].reshape(count // 2, PAD, 128)
            hs[h, 0, 0, begin // 2 : (begin + count) // 2] = own.astype(jnp.bfloat16)

    def down(n):
        begin, count = SPANS[n]
        parts = []
        for t in range(16):
            pair = [hs[h, o, i, begin // 2 : (begin + count) // 2] for h, (o, i) in enumerate(slots(t))]
            pair = jnp.concatenate(pair, axis=0).astype(jnp.float32).reshape(count * PAD, 128)
            parts.append(pair.astype(jnp.bfloat16))
        result = dot(jnp.concatenate(parts, axis=1), wd[...])
        back[begin : begin + count] = result.reshape(count, PAD, 256).astype(jnp.bfloat16)
        for i in range(SPANS[n][0], sum(SPANS[n])):
            if i == 0:
                own_back.start()
            else:
                giveback(i).start()

    def along(s):
        up, dn = (NZ - s) % NZ, s
        if s < 7:
            return [
                remote(kv.at[up, 0], kv.at[(NZ - s - 1) % NZ, 0], sent.at[5], kz_r.at[0, s], partner(1, 0)),
                remote(kv.at[dn, 0], kv.at[s + 1, 0], sent.at[5], kz_r.at[1, s], partner(-1, 0)),
            ]
        lo, hi = pl.ds(0, 128), pl.ds(128, 128)
        return [
            remote(kv.at[up, 0, lo], kv.at[8, 0, lo], sent.at[5], kz_r.at[0, s], partner(1, 0)),
            remote(kv.at[dn, 0, hi], kv.at[8, 0, hi], sent.at[5], kz_r.at[1, s], partner(-1, 0)),
        ]

    def across(r):
        return remote(kv.at[r, 0], kv.at[r, 1], sent.at[6], kd_r.at[r], partner(0, 1))

    def absorb(r):
        blocks = kv[r]
        stored = blocks[:, 0:128, :].reshape(256, 128)
        scores = jnp.concatenate(
            [dot(stored, q1[...], ((1,), (1,))), dot(stored, q2[...], ((1,), (1,)))], axis=0
        )
        new_max = jnp.maximum(run_max[...], jnp.max(scores, axis=0, keepdims=True))
        factor = jnp.exp(run_max[...] - new_max)
        raw = jnp.exp(scores - new_max)
        run_sum[...] = run_sum[...] * factor + jnp.sum(raw, axis=0, keepdims=True)
        turned_values = jnp.concatenate(
            [blocks[0, 128:192], blocks[1, 128:192], blocks[0, 192:256], blocks[1, 192:256]], axis=1
        )
        run_acc[...] = run_acc[...] * factor + dot(turned_values, raw.astype(jnp.bfloat16))
        run_max[...] = new_max

    def ring_step(s):
        if s > 0:
            for copy in along(s - 1):
                copy.wait_recv()
        if s < 8:
            for copy in along(s):
                copy.start()
        if 0 < s < 8:
            across(NZ - s).start()
        across(s).start()

    def attend(s):
        across(s).wait_recv()
        if s in (0, 8):
            absorb(s)
        else:
            across(NZ - s).wait_recv()

            def body(k, carry):
                absorb(s + k * (NZ - 2 * s))
                return carry

            lax.fori_loop(0, 2, body, 0)

    def heads():
        result = run_acc[...] / run_sum[...]
        result = jnp.concatenate([result[:, 0:TOK], result[:, TOK:]], axis=0).T.astype(jnp.bfloat16)
        ho[0, 0, 0] = result[0:128]
        ho[1, 0, 0] = result[128:256]

    def mix():
        parts, squares = [], None
        for t in range(16):
            part = jnp.concatenate([ho[h, o, i] for h, (o, i) in enumerate(slots(t))], axis=0).astype(jnp.float32)
            squares = part * part if squares is None else squares + part * part
            parts.append((part * mg_ref[pl.ds(t, 1), :]).astype(jnp.bfloat16))
        total = dot(jnp.concatenate(parts, axis=1), wo[...])
        scale = lax.rsqrt(jnp.sum(squares, axis=1, keepdims=True) / QDIM + EPS)
        att_ref[...] = (total * scale).astype(jnp.bfloat16)

    def combine():
        own_back.wait()
        arrived(ret.at[pl.ds(1, EXPERTS - 1)], ret_r.at[0])
        rows = ret[...].astype(jnp.float32).reshape(EXPERTS * PAD, 256).astype(jnp.bfloat16)
        same = lax.broadcasted_iota(jnp.int32, (TOK, TOK), 0) == lax.broadcasted_iota(jnp.int32, (TOK, TOK), 1)
        total = None
        for k in range(2):
            weight = jnp.sum(jnp.where(same, rw_ref[k : k + 1, :], 0.0), axis=1, keepdims=True)
            term = dot(pick[k], rows, ((0,), (0,))) * weight
            total = term if total is None else total + term
        mix_ref[...] = total.astype(jnp.bfloat16)

    for name in ORDER:
        kind, n, step = name[0], int(name[1:2] or 0), int(name[2:] or 0)
        if kind == "S":
            stage_s(n)
        elif kind == "A":
            stage_a(n)
        elif kind == "X":
            go(gx[n], step)
        elif kind == "E":
            go(gx[n], 6)
            feed_forward(n)
            go(gh[n], 0)
        elif kind == "H":
            go(gh[n], step)
        elif kind == "J":
            go(gh[n], 6)
            down(n)
        elif kind == "K":
            ring_step(n)
        elif kind == "T":
            attend(n)
        elif kind == "M":
            if n == 0:
                heads()
            go(gm, n)
            if n == 6:
                mix()
        elif kind == "Q":
            queries_and_keys()
        elif kind == "L":
            loads[n].wait()
        else:
            combine()

    left(out.at[:, pl.ds(1, EXPERTS - 1)], sent.at[0])
    left(back.at[pl.ds(1, EXPERTS - 1)], sent.at[1])
    left(xs.at[:, :, :, pl.ds(0, 30)], sent.at[2])
    left(hs.at[:, :, :, pl.ds(0, 15)], sent.at[3])
    left(xs.at[:, :, 0, pl.ds(0, 20)], sent.at[4])
    left(kv.at[pl.ds(1, NZ - 1), 0], sent.at[5])
    left(kv.at[:, 0], sent.at[6])


def shards(
    queries, key_rows, values, query_gain, key_gain, mix_gain, out_weight, expert_input, expert_gain, route_ids,
    route_weights, expert_gate, expert_up, expert_down,
):
    by_row, by_col = angle_tables()
    operands = (
        route_ids.T, expert_input, queries, key_rows.T, values.T, query_gain.reshape(1, HEAD), key_gain.reshape(1, HEAD),
        jnp.asarray(by_row), jnp.asarray(by_col), mix_gain.reshape(16, 128), expert_gain.reshape(32, 128),
        route_weights.T, out_weight, expert_gate, expert_up, expert_down,
    )
    vmem = pl.BlockSpec(memory_space=pltpu.VMEM)
    hbm = pl.BlockSpec(memory_space=pl.ANY)
    bf16, f32 = jnp.bfloat16, jnp.float32
    sem = pltpu.SemaphoreType.DMA
    return pl.pallas_call(
        kernel,
        out_shape=(pltpu.VMEM((TOK, 256), bf16), pltpu.VMEM((TOK, 256), bf16)),
        in_specs=[hbm] * 16,
        out_specs=(vmem, vmem),
        scratch_shapes=[
            *(pltpu.VMEM(a.shape, a.dtype) for a in operands[:12]),
            pltpu.VMEM((2, 128), f32),
            pltpu.VMEM((2, TOK, 128), f32),
            pltpu.VMEM((2 * TOK, 128), bf16),
            pltpu.VMEM((2 * TOK, 128), bf16),
            pltpu.VMEM((NZ, 2, 256, 128), bf16),
            pltpu.VMEM((1, 2 * TOK), f32),
            pltpu.VMEM((1, 2 * TOK), f32),
            pltpu.VMEM((HEAD, 2 * TOK), f32),
            pltpu.VMEM((2, EXPERTS * PAD, TOK), bf16),
            pltpu.VMEM((2, EXPERTS, PAD, 128), bf16),
            pltpu.VMEM((2, NX, NX, EXPERTS, PAD, 128), bf16),
            pltpu.VMEM((2, NX, NX, EXPERTS // 2, PAD, 128), bf16),
            pltpu.VMEM((2, NX, NX, 128, 128), bf16),
            pltpu.VMEM((EXPERTS, PAD, 256), bf16),
            pltpu.VMEM((EXPERTS, PAD, 256), bf16),
            pltpu.VMEM((MOST, 256), f32),
            pltpu.VMEM((MOST, 128), f32),
            pltpu.VMEM((D, 256), bf16),
            pltpu.VMEM((QDIM, 256), bf16),
            pltpu.VMEM((QDIM, 256), bf16),
            sem((7,)),
            sem((CHUNKS,)),
            sem((1,)),
            sem((2 * CHUNKS + 1, 6)),
            sem((2, 8)),
            sem((NZ,)),
            sem((4,)),
            sem((2,)),
            sem((12,)),
        ],
        compiler_params=pltpu.CompilerParams(
            collective_id=0, has_side_effects=True, vmem_limit_bytes=60 * 1024 * 1024
        ),
    )(*operands)


def solution(mesh):
    torus = Mesh(mesh.devices.reshape(NZ, 2, NX, NX), EP + TP)
    return jax.shard_map(
        shards,
        mesh=torus,
        in_specs=(
            P(EP, TP), P(EP, TP), P(EP, TP), P(), P(), P(), P(None, TP), P(EP, TP), P(), P(EP, None), P(EP, None),
            P(EP, None, TP), P(EP, None, TP), P(EP, None, TP),
        ),
        out_specs=(P(EP, TP), P(EP, TP)),
        check_vma=False,
    )
```

```python
import functools

import jax
import jax.numpy as jnp
import numpy as np
from jax import lax
from jax.experimental import pallas as pl
from jax.experimental.pallas import tpu as pltpu
from jax.sharding import Mesh
from jax.sharding import PartitionSpec as P

MESH = pl.DeviceIdType.MESH
EP = ("z", "c")
TP = ("y", "x")
HEAD = 64
GRID_W = 64
EPS = 1e-06
THETA = 10000.0
NZ = 16
NX = 4
TOK = 256
CAP = 22
PAD = 24
EXPERTS = 32
D = 4096
QDIM = 2048

OFFSETS = ((0, 1), (-1, 2), (3, -3), (4, -4), (5, -5), (6, -6), (7, -7), (8, -2))
CHUNKS = len(OFFSETS)
BLOCKS = [(dz, dc) for part in OFFSETS for dz in part for dc in (0, 1)]
SPANS = [(2 * sum(map(len, OFFSETS[:n])), 2 * len(OFFSETS[n])) for n in range(CHUNKS)]

BLOCKS_PER = 4
ROWS = BLOCKS_PER * CAP
TILES = ROWS // 8
HALF = (TILES + 1) // 2

ORDER = (
    "S0", "S1", "S2", "S3", "Q", "A0", "S5", "S6", "A1", "X02", "A2", "X01", "X11", "K0", "A3", "S7", "X21", "X03",
    "X04", "T0", "A5", "K1", "X14", "X13", "X31", "S4", "X05", "X32", "A6", "X51", "X12", "K2", "X33", "X52", "X15",
    "X34", "X61", "X53", "A7", "K3", "X23", "X35", "A4", "X63", "X54", "X62", "X55", "X71", "T1", "K4", "L0", "L1",
    "E3", "X41", "T2", "X65", "E5", "X73", "X64", "H31", "K5", "X22", "X72", "T3", "X43", "X74", "T4", "X75", "H51",
    "X44", "E6", "X25", "X24", "X42", "E1", "K6", "X45", "T5", "H33", "E7", "H32", "H53", "H61", "H34", "E0", "E2",
    "K7", "E4", "H35", "H71", "T6", "H52", "H55", "H63", "H54", "H64", "T7", "H11", "K8", "H21", "H41", "L2", "J3",
    "H73", "H62", "T8", "H65", "M0", "J5", "H72", "H74", "H12", "H13", "H43", "H44", "H75", "H24", "H01", "H14",
    "H42", "J6", "H23", "M1", "H45", "J7", "H03", "H22", "M2", "H15", "H25", "M3", "M4", "H02", "J4", "H04", "H05",
    "J2", "M5", "J1", "J0", "L3", "M6", "R",
)


def angle_tables():
    half = HEAD // 2
    inverse = (np.float32(THETA) ** (-np.arange(0, half, 2, dtype=np.float32) / np.float32(half))).astype(np.float32)
    angles = (np.arange(128, dtype=np.float32)[:, None] * inverse).astype(np.float32).astype(np.float64)
    pair = np.repeat(np.stack([np.cos(angles), np.sin(angles)]), 2, axis=2).astype(np.float32)
    pair[1, :, 0::2] *= -1
    none = np.zeros_like(pair)
    by_row = np.concatenate([pair, none, pair, none], axis=2)
    by_col = np.concatenate([none, pair, none, pair], axis=2)[:, :GRID_W]
    return by_row, by_col


def wrap(a, n):
    return lax.rem(a + n, n)


def norm_turn(x, gain, cosine, sine):
    low = lax.broadcasted_iota(jnp.int32, x.shape, 1) < HEAD
    squares = x * x
    first = jnp.sum(jnp.where(low, squares, 0.0), axis=1, keepdims=True)
    second = jnp.sum(jnp.where(low, 0.0, squares), axis=1, keepdims=True)
    x = x * lax.rsqrt(jnp.where(low, first, second) / HEAD + EPS) * gain
    even = lax.rem(lax.broadcasted_iota(jnp.int32, x.shape, 1), 2) == 0
    other = jnp.where(even, pltpu.roll(x, 127, 1), pltpu.roll(x, 1, 1))
    return x * cosine + other * sine


def dot(a, b, dims=((1,), (0,))):
    return lax.dot_general(a, b, (dims, ((), ())), preferred_element_type=jnp.float32)


def kernel(
    *refs,
):
    sources, (wo_hbm, wg_hbm, wu_hbm, wd_hbm) = refs[:12], refs[12:16]
    (att_ref, mix_ref), held = refs[16:18], refs[18:30]
    (
        gains, cs, q1, q2, kv, run_max, run_sum, run_acc, pick, out, land, xs, hs, ho, back, ret, wgu, wd, wo,
        sent, disp_r, ret_r, ag_r, kz_r, kd_r, w_s, own_s, in_s,
    ) = refs[30:]
    ids_ref, x_ref, q_ref, kt_ref, vt_ref, qg_ref, kg_ref, byrow_ref, bycol_ref, mg_ref, eg_ref, rw_ref = held
    z, c = lax.axis_index("z"), lax.axis_index("c")
    y, x = lax.axis_index("y"), lax.axis_index("x")
    coord = {"y": y, "x": x}

    barrier = pltpu.get_barrier_semaphore()

    def partner(dz, dc):
        return {"z": lax.rem(z + (dz + NZ), NZ), "c": lax.rem(c + dc, 2)}

    def side(axis, step):
        return {axis: lax.rem(coord[axis] + (step + NX), NX)}

    for dz, dc in sorted(BLOCKS[1:], key=lambda block: -abs(block[0])):
        pl.semaphore_signal(barrier, inc=1, device_id=partner(dz, dc), device_id_type=MESH)
    for axis in ("x", "y"):
        for step in (1, -1):
            pl.semaphore_signal(barrier, inc=1, device_id=side(axis, step), device_id_type=MESH)

    inputs = [pltpu.make_async_copy(src, dst, in_s.at[k]) for k, (src, dst) in enumerate(zip(sources, held))]
    for load in inputs:
        load.start()
    loads = [
        pltpu.make_async_copy(wg_hbm.at[0], wgu.at[:, 0:128], w_s.at[0]),
        pltpu.make_async_copy(wu_hbm.at[0], wgu.at[:, 128:256], w_s.at[1]),
        pltpu.make_async_copy(wd_hbm.at[0], wd, w_s.at[2]),
        pltpu.make_async_copy(wo_hbm, wo, w_s.at[3]),
    ]

    for load in inputs[:2]:
        load.wait()
    for load in loads:
        load.start()

    experts = lax.broadcasted_iota(jnp.int32, (EXPERTS, TOK), 0)
    hits = [jnp.where(experts == ids_ref[k : k + 1, :], 1.0, 0.0) for k in range(2)]
    earlier = lax.broadcasted_iota(jnp.int32, (TOK, TOK), 0) < lax.broadcasted_iota(jnp.int32, (TOK, TOK), 1)
    before = dot((hits[0] + hits[1]).astype(jnp.bfloat16), jnp.where(earlier, 1.0, 0.0).astype(jnp.bfloat16))
    keys = [
        ids_ref[k : k + 1, :].astype(jnp.float32) * 32.0 + jnp.sum(hits[k] * before, axis=0, keepdims=True)
        for k in range(2)
    ]
    places = lax.broadcasted_iota(jnp.int32, (PAD, TOK), 0)
    for n in range(CHUNKS):
        wanted = []
        begin, count = SPANS[n]
        for dz, dc in BLOCKS[begin : begin + count]:
            to = partner(dz, dc)
            wanted.append((places + (to["z"] * 2 + to["c"]) * 32).astype(jnp.float32))
        wanted = jnp.concatenate(wanted, axis=0)
        rows = pl.ds(begin * PAD, count * PAD)
        marks = [jnp.where(wanted == keys[k], 1.0, 0.0) for k in range(2)]
        for k in range(2):
            pick[k, rows, :] = marks[k].astype(jnp.bfloat16)
        chosen = dot((marks[0] + marks[1]).astype(jnp.bfloat16), x_ref[...])
        for h in range(2):
            out[h, begin : begin + count] = (
                chosen[:, h * 128 : (h + 1) * 128].reshape(count, PAD, 128).astype(jnp.bfloat16)
            )

    pl.semaphore_wait(barrier, len(BLOCKS) - 1 + 4)

    def arrived(ref, sem):
        remote(ref, ref, sem, sem, partner(0, 1)).wait_recv()

    def left(ref, sem):
        remote(ref, ref, sem, sem, partner(0, 1)).wait_send()

    def remote(src, dst, send, recv, device):
        return pltpu.make_async_remote_copy(
            src_ref=src, dst_ref=dst, send_sem=send, recv_sem=recv, device_id=device, device_id_type=MESH
        )

    chunk_of = [n for n, (begin, count) in enumerate(SPANS) for k in range(count)]

    def dispatch(i):
        return remote(out.at[:, i], land.at[:, i], sent.at[0], disp_r.at[chunk_of[i]], partner(*BLOCKS[i]))

    def giveback(i):
        dz, dc = BLOCKS[i]
        return remote(back.at[i], ret.at[i], sent.at[1], ret_r.at[0], partner(-dz, dc))

    own_out = pltpu.make_async_copy(out.at[:, 0], land.at[:, 0], own_s.at[0])
    own_back = pltpu.make_async_copy(back.at[0], ret.at[0], own_s.at[1])

    def queries_and_keys():
        for load in inputs[2:]:
            load.wait()
        first_row = (z * 2 + c) * (TOK // GRID_W)
        for g in range(TOK // GRID_W):
            for t in range(2):
                cs[t, g * GRID_W : (g + 1) * GRID_W, :] = byrow_ref[t, pl.ds(first_row + g, 1), :] + bycol_ref[t]
        for t, ref in enumerate((qg_ref, kg_ref)):
            gains[t : t + 1, 0:HEAD] = ref[...]
            gains[t : t + 1, HEAD:128] = ref[...]
        low = lax.broadcasted_iota(jnp.int32, (128, 128), 1) < HEAD
        keys_raw = kt_ref[...].astype(jnp.float32)
        keys_raw = jnp.concatenate([keys_raw[:, 0:128], keys_raw[:, 128:256]], axis=0).T
        kv[0, 0, 0:128, :] = norm_turn(
            keys_raw, gains[1:2, :], jnp.where(low, cs[0, 0:128], cs[0, 128:256]), jnp.where(low, cs[1, 0:128], cs[1, 128:256])
        ).astype(jnp.bfloat16)
        kv[0, 0, 128:192, :] = vt_ref[:, 0:128]
        kv[0, 0, 192:256, :] = vt_ref[:, 128:256]
        turned = norm_turn(q_ref[...].astype(jnp.float32), gains[0:1, :], cs[0], cs[1])
        turned = turned.astype(jnp.bfloat16).astype(jnp.float32) * 0.125
        low = lax.broadcasted_iota(jnp.int32, (TOK, 128), 1) < HEAD
        crossed = pltpu.roll(turned, HEAD, 1)
        q1[0:TOK, :] = jnp.where(low, turned, 0.0).astype(jnp.bfloat16)
        q1[TOK:, :] = jnp.where(low, crossed, 0.0).astype(jnp.bfloat16)
        q2[0:TOK, :] = jnp.where(low, 0.0, crossed).astype(jnp.bfloat16)
        q2[TOK:, :] = jnp.where(low, 0.0, turned).astype(jnp.bfloat16)
        run_max[...] = jnp.full_like(run_max, -jnp.inf)
        run_sum[...] = jnp.zeros_like(run_sum)
        run_acc[...] = jnp.zeros_like(run_acc)

    def stage_s(n):
        for i in range(SPANS[n][0], sum(SPANS[n])):
            if i == 0:
                own_out.start()
            else:
                dispatch(i).start()

    kinds = (0, 0, 1, 1, 2, 2, 3, 3, 5, 5, 4, 4, 5, 5, 5, 5)

    def gather(buf, begin, count, half, index, send):
        inner, outer = ("x", "y") if half == 0 else ("y", "x")
        lo, hi, whole = pl.ds(begin, count // 2), pl.ds(begin + count // 2, count - count // 2), pl.ds(begin, count)

        def at(o, i, part=whole):
            return buf.at[half, o, i, part]

        def copy(k, src, dst, axis, step):
            return remote(src, dst, sent.at[send + (k in (4, 5, 8, 9, 14, 15))], ag_r.at[index, kinds[k]], side(axis, step))

        both = pl.ds(1, 2)
        return [
            copy(0, at(0, 0), at(0, 2), inner, 1),
            copy(1, at(0, 0), at(0, 1), inner, -1),
            copy(2, at(0, 0), at(2, 0), outer, 1),
            copy(3, at(0, 0), at(1, 0), outer, -1),
            copy(4, at(0, 2, lo), at(0, 3, lo), inner, 1),
            copy(5, at(0, 1, hi), at(0, 3, hi), inner, -1),
            copy(6, at(0, both), at(2, both), outer, 1),
            copy(7, at(0, both), at(1, both), outer, -1),
            copy(8, at(2, 0, lo), at(3, 0, lo), outer, 1),
            copy(9, at(1, 0, hi), at(3, 0, hi), outer, -1),
            copy(10, at(0, 3), at(2, 3), outer, 1),
            copy(11, at(0, 3), at(1, 3), outer, -1),
            copy(12, at(2, 1), at(3, 1), outer, 1),
            copy(13, at(1, 2), at(3, 2), outer, -1),
            copy(14, at(2, 3, lo), at(3, 3, lo), outer, 1),
            copy(15, at(1, 3, hi), at(3, 3, hi), outer, -1),
        ]

    def both_halves(buf, begin, count, index, send):
        part, middle = pl.ds(begin, count), pl.ds(1, 2)
        landed = (
            buf.at[:, 0, middle, part], buf.at[:, middle, 0, part], buf.at[:, 0, 3, part],
            buf.at[:, middle, middle, part], buf.at[:, middle, 3, part], buf.at[:, 3, :, part],
        )
        return [gather(buf, begin, count, h, index, send) for h in range(2)], landed, index

    gx = [both_halves(xs, n * TILES, TILES, n, 2) for n in range(CHUNKS)]
    gh = [both_halves(hs, n * HALF, HALF, CHUNKS + n, 4) for n in range(CHUNKS)]
    gm = both_halves(ho, 0, 128, CHUNKS * 2, 6)

    steps = ((0, 1, 2, 3), (4, 5, 6, 7), (8, 9), (10, 11), (12, 13), (14, 15), ())

    def go(pair, step):
        gathers, landed, index = pair
        if step:
            arrived(landed[step - 1], ag_r.at[index, step - 1])
        for g in gathers:
            for k in steps[step]:
                g[k].start()

    def slots(t):
        ry, rx = (r + r // 2 - 2 * (r // 3) for r in (wrap(t // NX - y, NX), wrap(lax.rem(t, NX) - x, NX)))
        return (ry, rx), (rx, ry)

    def stage_a(n):
        begin, count = SPANS[n]
        if n == 0:
            own_out.wait()
            begin, count = 1, count - 1
        arrived(land.at[:, pl.ds(begin, count)], disp_r.at[n])
        for h in range(2):
            rows = [land[h, SPANS[n][0] + b].astype(jnp.float32)[0:CAP] for b in range(BLOCKS_PER)]
            rows = jnp.concatenate(rows, axis=0).reshape(TILES, 8, 128)
            xs[h, 0, 0, n * TILES : (n + 1) * TILES] = rows.astype(jnp.bfloat16)
        go(gx[n], 0)

    def feed_forward(n):
        parts, squares = [], None
        for t in range(16):
            for h, (o, i) in enumerate(slots(t)):
                part = xs[h, o, i, n * TILES : (n + 1) * TILES].astype(jnp.float32).reshape(ROWS, 128)
                squares = part * part if squares is None else squares + part * part
                parts.append((part * eg_ref[2 * t + h : 2 * t + h + 1, :]).astype(jnp.bfloat16))
        total = dot(jnp.concatenate(parts, axis=1), wgu[...])
        stat = lax.rsqrt(jnp.sum(squares, axis=1, keepdims=True) / D + EPS)
        gate = total[:, 0:128] * stat
        up = total[:, 128:256] * stat
        hidden = gate / (1.0 + jnp.exp(-gate)) * up
        for h in range(2):
            own = hidden[h * (ROWS - HALF * 8) :][0 : HALF * 8].reshape(HALF, 8, 128)
            hs[h, 0, 0, n * HALF : (n + 1) * HALF] = own.astype(jnp.bfloat16)

    def down(n):
        begin, count = SPANS[n]
        parts = []
        for t in range(16):
            pair = [hs[h, o, i, n * HALF + h : (n + 1) * HALF] for h, (o, i) in enumerate(slots(t))]
            pair = jnp.concatenate(pair, axis=0).astype(jnp.float32).reshape(ROWS, 128)
            parts.append(pair.astype(jnp.bfloat16))
        result = dot(jnp.concatenate(parts, axis=1), wd[...])
        none = jnp.zeros((PAD - CAP, 256), jnp.float32)
        rows = [r for b in range(BLOCKS_PER) for r in (result[b * CAP : (b + 1) * CAP], none)]
        back[begin : begin + count] = jnp.concatenate(rows, axis=0).reshape(count, PAD, 256).astype(jnp.bfloat16)
        for i in range(SPANS[n][0], sum(SPANS[n])):
            if i == 0:
                own_back.start()
            else:
                giveback(i).start()

    def along(s):
        up, dn = (NZ - s) % NZ, s
        if s < 7:
            return [
                remote(kv.at[up, 0], kv.at[(NZ - s - 1) % NZ, 0], sent.at[8], kz_r.at[0, s], partner(1, 0)),
                remote(kv.at[dn, 0], kv.at[s + 1, 0], sent.at[8], kz_r.at[1, s], partner(-1, 0)),
            ]
        lo, hi = pl.ds(0, 128), pl.ds(128, 128)
        return [
            remote(kv.at[up, 0, lo], kv.at[8, 0, lo], sent.at[8], kz_r.at[0, s], partner(1, 0)),
            remote(kv.at[dn, 0, hi], kv.at[8, 0, hi], sent.at[8], kz_r.at[1, s], partner(-1, 0)),
        ]

    def across(r):
        return remote(kv.at[r, 0], kv.at[r, 1], sent.at[9], kd_r.at[r], partner(0, 1))

    def absorb(rs):
        pairs = [(r, core) for r in rs for core in range(2)]
        stored = jnp.concatenate([kv[r, core, 0:128, :] for r, core in pairs], axis=0)
        scores = jnp.concatenate(
            [dot(stored, q1[...], ((1,), (1,))), dot(stored, q2[...], ((1,), (1,)))], axis=0
        )
        new_max = jnp.maximum(run_max[...], jnp.max(scores, axis=0, keepdims=True))
        factor = jnp.exp(run_max[...] - new_max)
        raw = jnp.exp(scores - new_max)
        run_sum[...] = run_sum[...] * factor + jnp.sum(raw, axis=0, keepdims=True)
        turned_values = jnp.concatenate(
            [kv[r, core, first : first + HEAD, :] for first in (128, 192) for r, core in pairs], axis=1
        )
        run_acc[...] = run_acc[...] * factor + dot(turned_values, raw.astype(jnp.bfloat16))
        run_max[...] = new_max

    def ring_step(s):
        if s > 0:
            for copy in along(s - 1):
                copy.wait_recv()
        if s < 8:
            for copy in along(s):
                copy.start()
        if 0 < s < 8:
            across(NZ - s).start()
        across(s).start()

    def attend(s):
        rs = (s,) if s in (0, 8) else (s, NZ - s)
        for r in rs:
            across(r).wait_recv()
        absorb(rs)

    def heads():
        result = run_acc[...] / run_sum[...]
        result = jnp.concatenate([result[:, 0:TOK], result[:, TOK:]], axis=0).T.astype(jnp.bfloat16)
        ho[0, 0, 0] = result[0:128]
        ho[1, 0, 0] = result[128:256]

    def mix():
        parts, squares = [], None
        for t in range(16):
            part = jnp.concatenate([ho[h, o, i] for h, (o, i) in enumerate(slots(t))], axis=0).astype(jnp.float32)
            squares = part * part if squares is None else squares + part * part
            parts.append((part * mg_ref[pl.ds(t, 1), :]).astype(jnp.bfloat16))
        total = dot(jnp.concatenate(parts, axis=1), wo[...])
        scale = lax.rsqrt(jnp.sum(squares, axis=1, keepdims=True) / QDIM + EPS)
        att_ref[...] = (total * scale).astype(jnp.bfloat16)

    def combine():
        own_back.wait()
        arrived(ret.at[pl.ds(1, EXPERTS - 1)], ret_r.at[0])
        rows = ret[...].astype(jnp.float32).reshape(EXPERTS * PAD, 256).astype(jnp.bfloat16)
        same = lax.broadcasted_iota(jnp.int32, (TOK, TOK), 0) == lax.broadcasted_iota(jnp.int32, (TOK, TOK), 1)
        total = None
        for k in range(2):
            weight = jnp.sum(jnp.where(same, rw_ref[k : k + 1, :], 0.0), axis=1, keepdims=True)
            term = dot(pick[k], rows, ((0,), (0,))) * weight
            total = term if total is None else total + term
        mix_ref[...] = total.astype(jnp.bfloat16)

    for name in ORDER:
        kind, n, step = name[0], int(name[1:2] or 0), int(name[2:] or 0)
        if kind == "S":
            stage_s(n)
        elif kind == "A":
            stage_a(n)
        elif kind == "X":
            go(gx[n], step)
        elif kind == "E":
            go(gx[n], 6)
            feed_forward(n)
            go(gh[n], 0)
        elif kind == "H":
            go(gh[n], step)
        elif kind == "J":
            go(gh[n], 6)
            down(n)
        elif kind == "K":
            ring_step(n)
        elif kind == "T":
            attend(n)
        elif kind == "M":
            if n == 0:
                heads()
            go(gm, n)
            if n == 6:
                mix()
        elif kind == "Q":
            queries_and_keys()
        elif kind == "L":
            loads[n].wait()
        else:
            combine()

    left(out.at[:, pl.ds(1, EXPERTS - 1)], sent.at[0])
    left(back.at[pl.ds(1, EXPERTS - 1)], sent.at[1])
    for k, buf in enumerate((xs, hs, ho)):
        left(buf.at[:, pl.ds(0, 3)], sent.at[2 + 2 * k])
        left(buf.at[:, 0, pl.ds(0, 3)], sent.at[3 + 2 * k])
    left(kv.at[pl.ds(1, NZ - 1), 0], sent.at[8])
    left(kv.at[:, 0], sent.at[9])


def shards(
    queries, key_rows, values, query_gain, key_gain, mix_gain, out_weight, expert_input, expert_gain, route_ids,
    route_weights, expert_gate, expert_up, expert_down,
):
    by_row, by_col = angle_tables()
    operands = (
        route_ids.T, expert_input, queries, key_rows.T, values.T, query_gain.reshape(1, HEAD), key_gain.reshape(1, HEAD),
        jnp.asarray(by_row), jnp.asarray(by_col), mix_gain.reshape(16, 128), expert_gain.reshape(32, 128),
        route_weights.T, out_weight, expert_gate, expert_up, expert_down,
    )
    vmem = pl.BlockSpec(memory_space=pltpu.VMEM)
    hbm = pl.BlockSpec(memory_space=pl.ANY)
    bf16, f32 = jnp.bfloat16, jnp.float32
    sem = pltpu.SemaphoreType.DMA
    return pl.pallas_call(
        kernel,
        out_shape=(pltpu.VMEM((TOK, 256), bf16), pltpu.VMEM((TOK, 256), bf16)),
        in_specs=[hbm] * 16,
        out_specs=(vmem, vmem),
        scratch_shapes=[
            *(pltpu.VMEM(a.shape, a.dtype) for a in operands[:12]),
            pltpu.VMEM((2, 128), f32),
            pltpu.VMEM((2, TOK, 128), f32),
            pltpu.VMEM((2 * TOK, 128), bf16),
            pltpu.VMEM((2 * TOK, 128), bf16),
            pltpu.VMEM((NZ, 2, 256, 128), bf16),
            pltpu.VMEM((1, 2 * TOK), f32),
            pltpu.VMEM((1, 2 * TOK), f32),
            pltpu.VMEM((HEAD, 2 * TOK), f32),
            pltpu.VMEM((2, EXPERTS * PAD, TOK), bf16),
            pltpu.VMEM((2, EXPERTS, PAD, 128), bf16),
            pltpu.VMEM((2, EXPERTS, PAD, 128), bf16),
            pltpu.VMEM((2, NX, NX, CHUNKS * TILES, 8, 128), bf16),
            pltpu.VMEM((2, NX, NX, CHUNKS * HALF, 8, 128), bf16),
            pltpu.VMEM((2, NX, NX, 128, 128), bf16),
            pltpu.VMEM((EXPERTS, PAD, 256), bf16),
            pltpu.VMEM((EXPERTS, PAD, 256), bf16),
            pltpu.VMEM((D, 256), bf16),
            pltpu.VMEM((QDIM, 256), bf16),
            pltpu.VMEM((QDIM, 256), bf16),
            sem((10,)),
            sem((CHUNKS,)),
            sem((1,)),
            sem((2 * CHUNKS + 1, 6)),
            sem((2, 8)),
            sem((NZ,)),
            sem((4,)),
            sem((2,)),
            sem((12,)),
        ],
        compiler_params=pltpu.CompilerParams(
            collective_id=0, has_side_effects=True, vmem_limit_bytes=60 * 1024 * 1024
        ),
    )(*operands)


def solution(mesh):
    torus = Mesh(mesh.devices.reshape(NZ, 2, NX, NX), EP + TP)
    return jax.shard_map(
        shards,
        mesh=torus,
        in_specs=(
            P(EP, TP), P(EP, TP), P(EP, TP), P(), P(), P(), P(None, TP), P(EP, TP), P(), P(EP, None), P(EP, None),
            P(EP, None, TP), P(EP, None, TP), P(EP, None, TP),
        ),
        out_specs=(P(EP, TP), P(EP, TP)),
        check_vma=False,
    )
```
